32 devices in a mesh: grp: 2 (over y), ra: 4 (over z), cb: 2 (over x), dp: 2 (over core).
Axes of the slice: x: 2, y: 2, z: 4, core: 2. Of those that a mesh axis runs over, the one named last changes fastest.
Arguments:
- tokens: bfloat16 [256, 2048], P(('grp', 'dp'), 'ra'), parts along dimension 0, may hold values from -51 to 51
- first_gain: float32 [2048], P('ra'), may hold values from 0.1 to 1.9
- first_gate: float32 [2048, 5632], P('ra', 'cb'), may hold values from -0.125 to 0.125
- first_up: float32 [2048, 5632], P('ra', 'cb'), may hold values from -0.125 to 0.125
- first_down: float32 [5632, 2048], P('cb', 'ra'), may hold values from -0.078125 to 0.078125
- first_gate_scale: float32 [5632], P('cb'), may hold values from 0.1 to 1.9
- first_up_scale: float32 [5632], P('cb'), may hold values from 0.1 to 1.9
- first_down_scale: float32 [2048], P('ra'), may hold values from 0.1 to 1.9
- second_gain: float32 [2048], P('ra'), may hold values from 0.1 to 1.9
- second_gate: float32 [2048, 5632], P('ra', 'cb'), may hold values from -0.125 to 0.125
- second_up: float32 [2048, 5632], P('ra', 'cb'), may hold values from -0.125 to 0.125
- second_down: float32 [5632, 2048], P('cb', 'ra'), may hold values from -0.078125 to 0.078125
- second_gate_scale: float32 [5632], P('cb'), may hold values from 0.1 to 1.9
- second_up_scale: float32 [5632], P('cb'), may hold values from 0.1 to 1.9
- second_down_scale: float32 [2048], P('ra'), may hold values from 0.1 to 1.9
Outputs:
- result: bfloat16 [256, 2048], P(('grp', 'dp'), 'ra'), parts along dimension 0
The draws below stay inside these ranges and needn't reach their ends.
There are 2 independent parts, one for each index of `grp`. The reference program is written for one: setup_inputs(seed, part) draws one part's arguments, and reference() takes and returns one part's arrays. A program takes and returns all parts, laid end to end along the dimension named above; an argument that names none is the same for every part. Nothing has to cross between parts.
All inputs are finite; a program needn't handle non-finite values.
Results may differ from the reference program's by a relative error of at most 0.04.
Values may be sent and summed in bfloat16 or wider, within the bound.
A program may use at most 64 MiB of HBM per device.

```python
import jax
import jax.numpy as jnp
from jax import lax

D = 2048
FF = 5632
TOKENS = 128
N_CB = 2


def draw_tokens(key, part):
    key_base = jax.random.fold_in(key, 11)
    key_rough = jax.random.fold_in(key, 12)
    columns = jnp.arange(D).astype(jnp.float32)
    rising = 3.0 ** (columns / D)
    rough = jnp.exp(jax.random.uniform(key_rough, (D,), jnp.float32, -0.35, 0.35))
    base = jnp.clip(jax.random.normal(key_base, (TOKENS, D), jnp.float32), -3.0, 3.0)
    return (base * rising * rough * 0.7).astype(jnp.bfloat16)


def steps_of(own_key, dims, shards, smallest, high):
    def one(position, parts):
        heights = jax.random.uniform(jax.random.fold_in(jax.random.fold_in(own_key, 6), position), (parts,), jnp.float32, smallest / len(shards), high / len(shards))
        return jnp.repeat(jnp.exp(heights), dims[position] // parts).reshape((-1,) + (1,) * (len(dims) - position - 1))

    factor_of = one(*shards[0])
    for cut in shards[1:]:
        factor_of = factor_of * one(*cut)
    return factor_of


def centred(stream_key, shape, scale, bound, pieces=(), dtype=jnp.bfloat16):
    result = scale * jax.random.normal(stream_key, shape, jnp.float32)
    if pieces:
        result = result * steps_of(stream_key, shape, pieces, -0.22, 0.18)
    return jnp.clip(result, -bound, bound).astype(dtype)


def setup_inputs(seed: int = 0, part: int = 0) -> dict:
    streams_of = jax.random.split(jax.random.key(seed), 16)
    own_keys = jax.random.split(jax.random.fold_in(streams_of[15], part), 16)
    tokens = draw_tokens(jax.random.fold_in(jax.random.fold_in(streams_of[15], part), 71), part)
    first_gain = jnp.clip(1.0 + 0.18 * jax.random.normal(streams_of[1], (D,), jnp.float32), 0.1, 1.9)
    first_gate = centred(streams_of[2], (D, FF), D ** -0.5, 0.125, ((0, 4), (1, 2)), jnp.float32)
    first_up = centred(streams_of[3], (D, FF), D ** -0.5, 0.125, ((0, 4), (1, 2)), jnp.float32)
    first_down = centred(streams_of[4], (FF, D), FF ** -0.5, 0.078125, ((0, 2), (1, 4)), jnp.float32)
    first_gate_scale = jnp.clip(1.0 + 0.18 * jax.random.normal(streams_of[5], (FF,), jnp.float32), 0.1, 1.9)
    first_up_scale = jnp.clip(1.0 + 0.18 * jax.random.normal(streams_of[6], (FF,), jnp.float32), 0.1, 1.9)
    first_down_scale = jnp.clip(1.0 + 0.18 * jax.random.normal(streams_of[7], (D,), jnp.float32), 0.1, 1.9)
    second_gain = jnp.clip(1.0 + 0.18 * jax.random.normal(streams_of[8], (D,), jnp.float32), 0.1, 1.9)
    second_gate = centred(streams_of[9], (D, FF), D ** -0.5, 0.125, ((0, 4), (1, 2)), jnp.float32)
    second_up = centred(streams_of[10], (D, FF), D ** -0.5, 0.125, ((0, 4), (1, 2)), jnp.float32)
    second_down = centred(streams_of[11], (FF, D), FF ** -0.5, 0.078125, ((0, 2), (1, 4)), jnp.float32)
    second_gate_scale = jnp.clip(1.0 + 0.18 * jax.random.normal(streams_of[12], (FF,), jnp.float32), 0.1, 1.9)
    second_up_scale = jnp.clip(1.0 + 0.18 * jax.random.normal(streams_of[13], (FF,), jnp.float32), 0.1, 1.9)
    second_down_scale = jnp.clip(1.0 + 0.18 * jax.random.normal(streams_of[14], (D,), jnp.float32), 0.1, 1.9)
    return dict(tokens=tokens, first_gain=first_gain, first_gate=first_gate, first_up=first_up, first_down=first_down, first_gate_scale=first_gate_scale, first_up_scale=first_up_scale, first_down_scale=first_down_scale, second_gain=second_gain, second_gate=second_gate, second_up=second_up, second_down=second_down, second_gate_scale=second_gate_scale, second_up_scale=second_up_scale, second_down_scale=second_down_scale)


EPS = 1e-06

def sublayer(values, gain, w_gate, w_up, w_down, gate_scale, up_scale, down_scale):
    floats = values.astype(jnp.float32)
    inverse = lax.rsqrt(lax.optimization_barrier(jnp.mean(floats * floats, axis=1, keepdims=True)) + EPS)
    scaled = (floats * gain).astype(jnp.bfloat16)
    gate = jnp.dot(scaled, w_gate.astype(jnp.bfloat16), preferred_element_type=jnp.float32) * gate_scale * inverse
    up_val = jnp.dot(scaled, w_up.astype(jnp.bfloat16), preferred_element_type=jnp.float32) * up_scale * inverse
    hidden = (jax.nn.silu(gate) * up_val).astype(jnp.bfloat16)
    block = FF // N_CB
    rows = hidden.shape[0]
    hidden_blocks = hidden.reshape(rows, N_CB, block).astype(jnp.float32)
    down_blocks = w_down.astype(jnp.bfloat16).reshape(N_CB, block, D).astype(jnp.float32)
    partial_terms = jnp.einsum('tcf,cfd->ctd', hidden_blocks, down_blocks).astype(jnp.bfloat16)
    partial_terms = lax.optimization_barrier(partial_terms)
    down = lax.optimization_barrier(jnp.sum(partial_terms.astype(jnp.float32), axis=0))
    return (0.3 * floats + 0.5 * down * down_scale).astype(jnp.bfloat16)

def reference(tokens, first_gain, first_gate, first_up, first_down, first_gate_scale, first_up_scale, first_down_scale, second_gain, second_gate, second_up, second_down, second_gate_scale, second_up_scale, second_down_scale):
    middle = sublayer(tokens, first_gain, first_gate, first_up, first_down, first_gate_scale, first_up_scale, first_down_scale)
    return sublayer(middle, second_gain, second_gate, second_up, second_down, second_gate_scale, second_up_scale, second_down_scale)
```

```python
import functools

import jax
import jax.numpy as jnp
from jax import lax
from jax.experimental import pallas as pl
from jax.experimental.pallas import tpu as pltpu
from jax.sharding import PartitionSpec as P

EPS = 1e-06
MESH = pl.DeviceIdType.MESH
LANES = 128
LAG = 5


def kernel(dims, *refs):
    n, m, cores, rows, width, units, pieces, total_width = dims
    (tokens, gain0, gate0, up0, down0, gs0, us0, ds0, gain1, gate1, up1, down1, gs1, us1, ds1) = refs[:15]
    out = refs[15]
    (values, scaled, vectors, scales, w_gu, w_down, own, sum_out, sum_in, cross_in, hid, acc, down_in, squares, inverse,
     small_sem, gu_sem, down_sem, sum_ss, sum_rs, cross_rs, hid_ss, hid_rs, part_ss, part_rs, sq_ss, sq_rs,
     turn_sem) = refs[16:]
    gate, up, down = (gate0, gate1), (up0, up1), (down0, down1)
    bf16, f32 = jnp.bfloat16, jnp.float32
    scope = jax.named_scope

    z, x, core = lax.axis_index("ra"), lax.axis_index("cb"), lax.axis_index("dp")
    lanes = pieces * LANES
    blocks = units // lanes
    half = n // 2
    owners = (half - 1, half)
    counts = (blocks - blocks // 2, blocks // 2)
    starts = (0, counts[0])
    left = z < half
    step = jnp.where(left, 1, -1)
    p = jnp.where(left, z, n - 1 - z)
    middle = (z == half - 1) | (z == half)
    first = jnp.where(left, counts[0], 0)
    n_far = jnp.where(left, counts[1], counts[0])
    n_near = blocks - n_far
    near_start = jnp.where(left, 0, counts[0])

    def wait(ref, sem):
        pltpu.make_async_copy(ref, ref, sem).wait()

    def columns(c):
        return pl.ds(pl.multiple_of(c * lanes, lanes), lanes)

    def gate_copy(l, c):
        return pltpu.make_async_copy(gate[l].at[:, columns(c)], w_gu.at[l, c, :, pl.ds(0, lanes)], gu_sem.at[c])

    def up_copy(l, c):
        return pltpu.make_async_copy(up[l].at[:, columns(c)], w_gu.at[l, c, :, pl.ds(lanes, lanes)], gu_sem.at[c])

    def down_copy(l, c):
        return pltpu.make_async_copy(down[l].at[columns(c), :], w_down.at[l, c], down_sem.at[c])

    def sum_copy(l, b):
        return pltpu.make_async_remote_copy(
            src_ref=sum_out.at[l, b], dst_ref=sum_in.at[l, b], send_sem=sum_ss.at[l], recv_sem=sum_rs.at[b],
            device_id={"ra": z + step}, device_id_type=MESH)

    def cross_copy(l, b):
        return pltpu.make_async_remote_copy(
            src_ref=sum_out.at[l, b], dst_ref=cross_in.at[l, b], send_sem=sum_ss.at[l],
            recv_sem=cross_rs.at[b - first * pieces], device_id={"ra": z + step}, device_id_type=MESH)

    def hid_copy(l, c, i, dest):
        part = hid.at[l, c, :, pl.ds(i * LANES, LANES)]
        return pltpu.make_async_remote_copy(
            src_ref=part, dst_ref=part, send_sem=hid_ss.at[l, dest], recv_sem=hid_rs.at[c],
            device_id={"ra": dest}, device_id_type=MESH)

    def part_copy(l, o, sender):
        return pltpu.make_async_remote_copy(
            src_ref=down_in.at[l, sender], dst_ref=down_in.at[l, sender], send_sem=part_ss.at[l, o],
            recv_sem=part_rs.at[l, sender], device_id={"cb": lax.rem(x + o, m)}, device_id_type=MESH)

    def sq_copy(l, end, sender):
        return pltpu.make_async_remote_copy(
            src_ref=squares.at[l, sender], dst_ref=squares.at[l, sender], send_sem=sq_ss.at[l, end],
            recv_sem=sq_rs, device_id={"ra": owners[end]}, device_id_type=MESH)

    def others():
        return [jnp.where(left, n - 1 - o, o) + jnp.where(
            left, jnp.where(n - 1 - o <= z, -1, 0), jnp.where(o >= z, 1, 0)) for o in range(n - 1)]

    def stream(j):
        return lax.rem(first + j, blocks)

    def loop(low, high, step_fn):
        def one(i, carry):
            step_fn(i)
            return carry
        lax.fori_loop(low, high, one, 0)

    urgent = [pltpu.make_async_copy(tokens, values, small_sem.at[0]),
              pltpu.make_async_copy(gain0, vectors.at[3], small_sem.at[1])]
    for copy in urgent:
        copy.start()

    def start_first(i):
        c = stream(i)
        gate_copy(0, c).start()
        up_copy(0, c).start()

    loop(0, blocks, start_first)
    for i, src in enumerate((ds0, gain1, ds1)):
        pltpu.make_async_copy(src, vectors.at[i], small_sem.at[2]).start()
    for i, src in enumerate((gs0, gs1, us0, us1)):
        pltpu.make_async_copy(src, scales.at[i], small_sem.at[3]).start()

    barrier = pltpu.get_barrier_semaphore()

    def greet(device):
        pl.semaphore_signal(barrier, inc=1, device_id={"ra": device}, device_id_type=MESH)

    @pl.when(middle)
    def _():
        for o in range(1, n):
            greet(lax.rem(z + o, n))

    @pl.when(jnp.logical_not(middle))
    def _():
        for owner in owners:
            greet(owner)

        @pl.when(p < half - 2)
        def _():
            greet(z + step)

        @pl.when(p > 0)
        def _():
            greet(z - step)

    for o in range(1, m):
        pl.semaphore_signal(barrier, inc=1, device_id={"cb": lax.rem(x + o, m)}, device_id_type=MESH)
    for o in range(1, cores):
        pl.semaphore_signal(barrier, inc=1, device_id={"dp": lax.rem(core + o, cores)}, device_id_type=MESH)
    with scope("small"):
        for copy in urgent:
            copy.wait()

    for l in range(2):
        scaled[...] = (values[...].astype(f32) * vectors[(3, 1)[l]]).astype(bf16)
        if l == 0:
            with scope("barrier"):
                greeted = jnp.where(middle, n - 1, 2 + jnp.where(p < half - 2, 1, 0) + jnp.where(p > 0, 1, 0))
                pl.semaphore_wait(barrier, greeted + m + cores - 2)

        def product(k, store):
            if l == 0:
                down_copy(0, stream(k)).start()
            c = stream(k)
            with scope("w_gu"):
                wait(w_gu.at[l, c], gu_sem.at[c])
            both = jnp.dot(scaled[...], w_gu[l, c].astype(bf16), preferred_element_type=f32)
            for i in range(pieces):
                a, b = i * LANES, lanes + i * LANES
                store(c * pieces + i, both[:, a:a + LANES], both[:, b:b + LANES])

        def send_squares(k):
            @pl.when(k == 1)
            def _():
                floats = values[...].astype(f32)
                squares[l, z] = lax.dot_general(
                    jnp.ones((8, width), f32), floats * floats, (((1,), (1,)), ((), ())),
                    precision=lax.Precision.HIGHEST, preferred_element_type=f32)
                for end in range(2):
                    @pl.when(z != owners[end])
                    def _():
                        sq_copy(l, end, z).start()

        def fetch_second():
            if l == 0:
                def one(k):
                    c = stream(k)
                    gate_copy(1, c).start()
                    up_copy(1, c).start()
                loop(0, blocks, one)

        def use_hidden(c):
            with scope("w_down"):
                down_copy(l, c).wait()
            acc[...] += jnp.dot(hid[l, c], w_down[l, c].astype(bf16), preferred_element_type=f32)

        def wait_hidden(c):
            with scope("w_hid"):
                wait(hid.at[l, c], hid_rs.at[c])

        def to_out(b, g, u):
            sum_out[l, b, :, :LANES] = g.astype(bf16)
            sum_out[l, b, :, LANES:] = u.astype(bf16)

        def to_own(b, g, u):
            own[b, :, :LANES] = g
            own[b, :, LANES:] = u

        def pass_on(b, copy):
            with scope("w_sum"):
                sum_copy(l, b).wait_recv()
            sum_out[l, b] = (own[b] + sum_in[l, b].astype(f32)).astype(bf16)
            copy(l, b).start()

        @pl.when(jnp.logical_not(middle))
        def _():
            @pl.when(p == 0)
            def _():
                def make(k):
                    product(k, to_out)
                    send = [sum_copy(l, stream(k) * pieces + i) for i in range(pieces)]
                    if l == 0:
                        @pl.when(core == 0)
                        def _():
                            for copy in send:
                                copy.start()
                    else:
                        for copy in send:
                            copy.start()
                    send_squares(k)

                with scope("make"):
                    loop(0, blocks, make)
                fetch_second()
                if l == 0:
                    @pl.when(core > 0)
                    def _():
                        with scope("turn"):
                            pl.semaphore_wait(turn_sem, 1)

                        def one(k):
                            for i in range(pieces):
                                sum_copy(l, stream(k) * pieces + i).start()
                        loop(0, blocks, one)

                    @pl.when(core < cores - 1)
                    def _():
                        with scope("held"):
                            wait(sum_out.at[l], sum_ss.at[l])
                        pl.semaphore_signal(turn_sem, inc=1, device_id={"dp": core + 1}, device_id_type=MESH)

            @pl.when(p > 0)
            def _():
                def relay(k):
                    product(k, to_own)
                    send_squares(k)
                    for i in range(pieces):
                        pass_on(stream(k) * pieces + i, sum_copy)

                loop(0, blocks, relay)
                fetch_second()

            acc[...] = jnp.zeros_like(acc)

            def gather(k):
                for d in range(2):
                    @pl.when(k < counts[d])
                    def _():
                        wait_hidden(starts[d] + k)
                        use_hidden(starts[d] + k)

            with scope("gather"):
                loop(0, counts[0], gather)

        @pl.when(middle)
        def _():
            ahead = blocks // 2

            def make(k):
                product(k, to_own)
                send_squares(k)

            with scope("make"):
                loop(0, ahead, make)

            def far(k):
                make(k)

                @pl.when(k - ahead < n_far)
                def _():
                    for i in range(pieces):
                        b = stream(k - ahead) * pieces + i
                        if half == 1:
                            sum_out[l, b] = own[b].astype(bf16)
                            cross_copy(l, b).start()
                        else:
                            pass_on(b, cross_copy)

            with scope("far"):
                loop(ahead, blocks, far)
            fetch_second()
            acc[...] = jnp.zeros_like(acc)
            with scope("w_sq"):
                wait(squares.at[l, pl.ds(0, n - 1)], sq_rs)
            every = squares[l].reshape(8 * n, rows)
            total = lax.dot_general(
                every, jnp.full((8 * n, LANES), 0.125, f32), (((0,), (0,)), ((), ())),
                precision=lax.Precision.HIGHEST, preferred_element_type=f32)
            inverse[...] = lax.rsqrt(total / total_width + EPS)
            if l == 0:
                with scope("w_small"):
                    wait(scales, small_sem.at[3])

            def near(s):
                @pl.when(s < n_near)
                def _():
                    c = near_start + s
                    for i in range(pieces):
                        b = c * pieces + i
                        both = own[b]
                        if half > 1:
                            with scope("w_sum"):
                                sum_copy(l, b).wait_recv()
                            both = both + sum_in[l, b].astype(f32)
                        with scope("w_cross"):
                            wait(cross_in.at[l, b], cross_rs.at[b - near_start * pieces])
                        both = both + cross_in[l, b].astype(f32)
                        inv = inverse[...]
                        g = both[:, :LANES] * scales[l, pl.ds(b, 1), :] * inv
                        u = both[:, LANES:] * scales[2 + l, pl.ds(b, 1), :] * inv
                        hid[l, c, :, i * LANES:(i + 1) * LANES] = (g / (1.0 + jnp.exp(-g)) * u).astype(bf16)
                        for dest in others():
                            hid_copy(l, c, i, dest).start()
                    use_hidden(c)

                k = s - LAG

                @pl.when((k >= 0) & (k < n_far))
                def _():
                    wait_hidden(first + k)
                    use_hidden(first + k)

            with scope("near"):
                loop(0, counts[0] + LAG, near)

        down_in[l, x] = acc[...].astype(bf16)
        for o in range(1, m):
            part_copy(l, o, x).start()
        if l == 0:
            loop(0, blocks, lambda k: down_copy(1, k).start())
            wait(vectors.at[pl.ds(0, 3)], small_sem.at[2])

            @pl.when(jnp.logical_not(middle))
            def _():
                wait(scales, small_sem.at[3])
        with scope("exch"):
            for o in range(1, m):
                part_copy(l, o, lax.rem(x + o, m)).wait_recv()
        total = down_in[l, 0].astype(f32)
        for o in range(1, m):
            total = total + down_in[l, o].astype(f32)
        result = (0.3 * values[...].astype(f32) + 0.5 * total * vectors[(0, 2)[l]]).astype(bf16)
        if l == 0:
            values[...] = result
        else:
            out[...] = result

    with scope("drain"):
        for l in range(2):
            for o in range(1, m):
                part_copy(l, o, x).wait_send()
            for end in range(2):
                @pl.when(z != owners[end])
                def _():
                    sq_copy(l, end, z).wait_send()

            kept = core == cores - 1 if l == 0 else True

            @pl.when(jnp.logical_not(middle) & (kept | (p > 0)))
            def _():
                wait(sum_out.at[l], sum_ss.at[l])

            for d in range(2):
                @pl.when(z == owners[d])
                def _():
                    wait(sum_out.at[l, pl.ds(0, counts[1 - d] * pieces)], sum_ss.at[l])
                    for dest in range(n):
                        if dest != owners[d]:
                            wait(hid.at[l, pl.ds(0, counts[d])], hid_ss.at[l, dest])


def per_device(n, m, cores, *args):
    tokens = args[0]
    rows, width = tokens.shape
    units = args[2].shape[1]
    pieces = 2 if units % (2 * LANES) == 0 else 1
    lanes = pieces * LANES
    blocks = units // lanes
    parts = units // LANES
    bf16, f32 = jnp.bfloat16, jnp.float32
    flat = [a if a.ndim > 1 else a.reshape(1, width) if i in (1, 7, 8, 14) else a.reshape(parts, LANES) for i, a in enumerate(args)]
    dma = pltpu.SemaphoreType.DMA
    return pl.pallas_call(
        functools.partial(kernel, (n, m, cores, rows, width, units, pieces, n * width)),
        out_shape=jax.ShapeDtypeStruct((rows, width), bf16),
        in_specs=[pl.BlockSpec(memory_space=pl.ANY)] * len(flat),
        out_specs=pl.BlockSpec(memory_space=pltpu.VMEM),
        scratch_shapes=[
            pltpu.VMEM((rows, width), bf16),
            pltpu.VMEM((rows, width), bf16),
            pltpu.VMEM((4, 1, width), f32),
            pltpu.VMEM((4, parts, LANES), f32),
            pltpu.VMEM((2, blocks, width, 2 * lanes), f32),
            pltpu.VMEM((2, blocks, lanes, width), f32),
            pltpu.VMEM((parts, rows, 2 * LANES), f32),
            pltpu.VMEM((2, parts, rows, 2 * LANES), bf16),
            pltpu.VMEM((2, parts, rows, 2 * LANES), bf16),
            pltpu.VMEM((2, parts, rows, 2 * LANES), bf16),
            pltpu.VMEM((2, blocks, rows, lanes), bf16),
            pltpu.VMEM((rows, width), f32),
            pltpu.VMEM((2, m, rows, width), bf16),
            pltpu.VMEM((2, n, 8, rows), f32),
            pltpu.VMEM((rows, LANES), f32),
            dma((4,)),
            dma((blocks,)),
            dma((blocks,)),
            dma((2,)),
            dma((parts,)),
            dma(((blocks - blocks // 2) * pieces,)),
            dma((2, n)),
            dma((blocks,)),
            dma((2, m)),
            dma((2, m)),
            dma((2, 2)),
            dma,
            pltpu.SemaphoreType.REGULAR,
        ],
        compiler_params=pltpu.CompilerParams(
            collective_id=0, has_side_effects=True, vmem_limit_bytes=60 * 1024 * 1024
        ),
    )(*flat)


def solution(mesh):
    in_specs = (
        P(("grp", "dp"), "ra"),
        P("ra"),
        P("ra", "cb"),
        P("ra", "cb"),
        P("cb", "ra"),
        P("cb"),
        P("cb"),
        P("ra"),
        P("ra"),
        P("ra", "cb"),
        P("ra", "cb"),
        P("cb", "ra"),
        P("cb"),
        P("cb"),
        P("ra"),
    )
    out_specs = P(("grp", "dp"), "ra")
    n, m, cores = mesh.shape["ra"], mesh.shape["cb"], mesh.shape["dp"]
    return jax.shard_map(
        functools.partial(per_device, n, m, cores), mesh=mesh, in_specs=in_specs, out_specs=out_specs, check_vma=False
    )
```

```python
import functools

import jax
import jax.numpy as jnp
from jax import lax
from jax.experimental import pallas as pl
from jax.experimental.pallas import tpu as pltpu
from jax.sharding import PartitionSpec as P

EPS = 1e-06
MESH = pl.DeviceIdType.MESH
LANES = 128
LAG = 5


def kernel(dims, *refs):
    n, m, cores, rows, width, units, pieces, total_width = dims
    (tokens, gain0, gate0, up0, down0, gs0, us0, ds0, gain1, gate1, up1, down1, gs1, us1, ds1) = refs[:15]
    out = refs[15]
    (values, scaled, vectors, scales, w_gu, w_down, own, sum_out, sum_in, cross_in, hid, acc, down_in, squares, inverse,
     small_sem, gu_sem, down_sem, sum_ss, sum_rs, cross_rs, hid_ss, hid_rs, part_ss, part_rs, sq_ss, sq_rs,
     turn_sem) = refs[16:]
    gate, up, down = (gate0, gate1), (up0, up1), (down0, down1)
    bf16, f32 = jnp.bfloat16, jnp.float32
    scope = jax.named_scope

    z, x, core = lax.axis_index("ra"), lax.axis_index("cb"), lax.axis_index("dp")
    lanes = pieces * LANES
    blocks = units // lanes
    half = n // 2
    owners = (half - 1, half)
    counts = (blocks - blocks // 2, blocks // 2)
    starts = (0, counts[0])
    left = z < half
    step = jnp.where(left, 1, -1)
    p = jnp.where(left, z, n - 1 - z)
    middle = (z == half - 1) | (z == half)
    first = jnp.where(left, counts[0], 0)
    n_far = jnp.where(left, counts[1], counts[0])
    n_near = blocks - n_far
    near_start = jnp.where(left, 0, counts[0])

    def wait(ref, sem):
        pltpu.make_async_copy(ref, ref, sem).wait()

    def columns(c):
        return pl.ds(pl.multiple_of(c * lanes, lanes), lanes)

    def gate_copy(l, c):
        return pltpu.make_async_copy(gate[l].at[:, columns(c)], w_gu.at[l, c, :, pl.ds(0, lanes)], gu_sem.at[c])

    def up_copy(l, c):
        return pltpu.make_async_copy(up[l].at[:, columns(c)], w_gu.at[l, c, :, pl.ds(lanes, lanes)], gu_sem.at[c])

    def down_copy(l, c):
        return pltpu.make_async_copy(down[l].at[columns(c), :], w_down.at[l, c], down_sem.at[c])

    def sum_copy(l, b):
        return pltpu.make_async_remote_copy(
            src_ref=sum_out.at[l, b], dst_ref=sum_in.at[l, b], send_sem=sum_ss.at[l], recv_sem=sum_rs.at[b],
            device_id={"ra": z + step}, device_id_type=MESH)

    def cross_copy(l, b):
        return pltpu.make_async_remote_copy(
            src_ref=sum_out.at[l, b], dst_ref=cross_in.at[l, b], send_sem=sum_ss.at[l],
            recv_sem=cross_rs.at[b - first * pieces], device_id={"ra": z + step}, device_id_type=MESH)

    def hid_copy(l, c, i, dest):
        part = hid.at[l, c, :, pl.ds(i * LANES, LANES)]
        return pltpu.make_async_remote_copy(
            src_ref=part, dst_ref=part, send_sem=hid_ss.at[l, dest], recv_sem=hid_rs.at[c],
            device_id={"ra": dest}, device_id_type=MESH)

    def part_copy(l, o, sender):
        return pltpu.make_async_remote_copy(
            src_ref=down_in.at[l, sender], dst_ref=down_in.at[l, sender], send_sem=part_ss.at[l, o - 1],
            recv_sem=part_rs.at[l, o - 1], device_id={"cb": lax.rem(x + o, m)}, device_id_type=MESH)

    def sq_copy(l, end, sender):
        return pltpu.make_async_remote_copy(
            src_ref=squares.at[l, sender], dst_ref=squares.at[l, sender], send_sem=sq_ss.at[l],
            recv_sem=sq_rs, device_id={"ra": owners[end]}, device_id_type=MESH)

    def others():
        return [jnp.where(left, n - 1 - o, o) + jnp.where(
            left, jnp.where(n - 1 - o <= z, -1, 0), jnp.where(o >= z, 1, 0)) for o in range(n - 1)]

    def stream(j):
        return lax.rem(first + j, blocks)

    def loop(low, high, step_fn):
        def one(i, carry):
            step_fn(i)
            return carry
        lax.fori_loop(low, high, one, 0)

    urgent = [pltpu.make_async_copy(tokens, values, small_sem.at[0]),
              pltpu.make_async_copy(gain0, vectors.at[3], small_sem.at[1])]
    for copy in urgent:
        copy.start()

    def start_first(i):
        c = stream(i)
        gate_copy(0, c).start()
        up_copy(0, c).start()

    loop(0, blocks, start_first)
    for i, src in enumerate((ds0, gain1, ds1)):
        pltpu.make_async_copy(src, vectors.at[i], small_sem.at[2]).start()
    for i, src in enumerate((gs0, gs1, us0, us1)):
        pltpu.make_async_copy(src, scales.at[i], small_sem.at[3]).start()

    barrier = pltpu.get_barrier_semaphore()

    def greet(device):
        pl.semaphore_signal(barrier, inc=1, device_id={"ra": device}, device_id_type=MESH)

    @pl.when(middle)
    def _():
        for o in range(1, n):
            greet(lax.rem(z + o, n))

    @pl.when(jnp.logical_not(middle))
    def _():
        for owner in owners:
            greet(owner)

        @pl.when(p < half - 2)
        def _():
            greet(z + step)

        @pl.when(p > 0)
        def _():
            greet(z - step)

    for o in range(1, m):
        pl.semaphore_signal(barrier, inc=1, device_id={"cb": lax.rem(x + o, m)}, device_id_type=MESH)
    for o in range(1, cores):
        pl.semaphore_signal(barrier, inc=1, device_id={"dp": lax.rem(core + o, cores)}, device_id_type=MESH)
    with scope("small"):
        for copy in urgent:
            copy.wait()

    for l in range(2):
        scaled[...] = (values[...].astype(f32) * vectors[(3, 1)[l]]).astype(bf16)
        if l == 0:
            with scope("barrier"):
                greeted = jnp.where(middle, n - 1, 2 + jnp.where(p < half - 2, 1, 0) + jnp.where(p > 0, 1, 0))
                pl.semaphore_wait(barrier, greeted + m + cores - 2)

        def product(k, store):
            if l == 0:
                down_copy(0, stream(k)).start()
            c = stream(k)
            with scope("w_gu"):
                wait(w_gu.at[l, c], gu_sem.at[c])
            both = jnp.dot(scaled[...], w_gu[l, c].astype(bf16), preferred_element_type=f32)
            for i in range(pieces):
                a, b = i * LANES, lanes + i * LANES
                store(c * pieces + i, both[:, a:a + LANES], both[:, b:b + LANES])

        def send_squares(k):
            @pl.when(k == 1)
            def _():
                floats = values[...].astype(f32)
                squares[l, z] = lax.dot_general(
                    jnp.ones((8, width), f32), floats * floats, (((1,), (1,)), ((), ())),
                    precision=lax.Precision.HIGHEST, preferred_element_type=f32)
                for end in range(2):
                    @pl.when(z != owners[end])
                    def _():
                        sq_copy(l, end, z).start()

        def fetch_second():
            if l == 0:
                def one(k):
                    c = stream(k)
                    gate_copy(1, c).start()
                    up_copy(1, c).start()
                loop(0, blocks, one)

        def use_hidden(c):
            down_copy(l, c).wait()
            acc[...] += jnp.dot(hid[l, c], w_down[l, c].astype(bf16), preferred_element_type=f32)

        def wait_hidden(c):
            with scope("w_hid"):
                wait(hid.at[l, c], hid_rs.at[c])

        def to_out(b, g, u):
            sum_out[l, b, :, :LANES] = g.astype(bf16)
            sum_out[l, b, :, LANES:] = u.astype(bf16)

        def to_own(b, g, u):
            own[b, :, :LANES] = g
            own[b, :, LANES:] = u

        def pass_on(b, copy):
            with scope("w_sum"):
                sum_copy(l, b).wait_recv()
            sum_out[l, b] = (own[b] + sum_in[l, b].astype(f32)).astype(bf16)
            copy(l, b).start()

        @pl.when(jnp.logical_not(middle))
        def _():
            @pl.when(p == 0)
            def _():
                def make(k):
                    product(k, to_out)
                    send = [sum_copy(l, stream(k) * pieces + i) for i in range(pieces)]
                    if l == 0:
                        @pl.when(core == 0)
                        def _():
                            for copy in send:
                                copy.start()
                    else:
                        for copy in send:
                            copy.start()
                    send_squares(k)

                with scope("make"):
                    loop(0, blocks, make)
                fetch_second()
                if l == 0:
                    @pl.when(core > 0)
                    def _():
                        with scope("turn"):
                            pl.semaphore_wait(turn_sem, 1)

                        def one(k):
                            for i in range(pieces):
                                sum_copy(l, stream(k) * pieces + i).start()
                        loop(0, blocks, one)

                    @pl.when(core < cores - 1)
                    def _():
                        with scope("held"):
                            wait(sum_out.at[l], sum_ss.at[l])
                        pl.semaphore_signal(turn_sem, inc=1, device_id={"dp": core + 1}, device_id_type=MESH)

            @pl.when(p > 0)
            def _():
                def relay(k):
                    product(k, to_own)
                    send_squares(k)
                    for i in range(pieces):
                        pass_on(stream(k) * pieces + i, sum_copy)

                loop(0, blocks, relay)
                fetch_second()

            acc[...] = jnp.zeros_like(acc)

            def gather(k):
                for d in range(2):
                    @pl.when(k < counts[d])
                    def _():
                        wait_hidden(starts[d] + k)
                        use_hidden(starts[d] + k)

            with scope("gather"):
                loop(0, counts[0], gather)

        @pl.when(middle)
        def _():
            ahead = blocks // 2

            def make(k):
                product(k, to_own)
                send_squares(k)

            with scope("make"):
                loop(0, ahead, make)

            def far(k):
                make(k)

                @pl.when(k - ahead < n_far)
                def _():
                    for i in range(pieces):
                        b = stream(k - ahead) * pieces + i
                        if half == 1:
                            sum_out[l, b] = own[b].astype(bf16)
                            cross_copy(l, b).start()
                        else:
                            pass_on(b, cross_copy)

            with scope("far"):
                loop(ahead, blocks, far)
            fetch_second()
            acc[...] = jnp.zeros_like(acc)
            with scope("w_sq"):
                wait(squares.at[l, pl.ds(0, n - 1)], sq_rs)
            every = squares[l].reshape(8 * n, rows)
            total = lax.dot_general(
                every, jnp.full((8 * n, LANES), 0.125, f32), (((0,), (0,)), ((), ())),
                precision=lax.Precision.HIGHEST, preferred_element_type=f32)
            inverse[...] = lax.rsqrt(total / total_width + EPS)
            if l == 0:
                with scope("w_small"):
                    wait(scales, small_sem.at[3])

            def near(s):
                @pl.when(s < n_near)
                def _():
                    c = near_start + s
                    for i in range(pieces):
                        b = c * pieces + i
                        both = own[b]
                        if half > 1:
                            with scope("w_sum"):
                                sum_copy(l, b).wait_recv()
                            both = both + sum_in[l, b].astype(f32)
                        with scope("w_cross"):
                            wait(cross_in.at[l, b], cross_rs.at[b - near_start * pieces])
                        both = both + cross_in[l, b].astype(f32)
                        inv = inverse[...]
                        g = both[:, :LANES] * scales[l, pl.ds(b, 1), :] * inv
                        u = both[:, LANES:] * scales[2 + l, pl.ds(b, 1), :] * inv
                        hid[l, c, :, i * LANES:(i + 1) * LANES] = (g / (1.0 + jnp.exp(-g)) * u).astype(bf16)
                        for dest in others():
                            hid_copy(l, c, i, dest).start()
                    use_hidden(c)

                k = s - LAG

                @pl.when((k >= 0) & (k < n_far))
                def _():
                    wait_hidden(first + k)
                    use_hidden(first + k)

            with scope("near"):
                loop(0, counts[0] + LAG, near)

        down_in[l, x] = acc[...].astype(bf16)
        for o in range(1, m):
            part_copy(l, o, x).start()
        if l == 0:
            loop(0, blocks, lambda k: down_copy(1, k).start())
            wait(vectors.at[pl.ds(0, 3)], small_sem.at[2])

            @pl.when(jnp.logical_not(middle))
            def _():
                wait(scales, small_sem.at[3])
        with scope("exch"):
            for o in range(1, m):
                part_copy(l, o, lax.rem(x - o + m, m)).wait_recv()
        total = down_in[l, 0].astype(f32)
        for o in range(1, m):
            total = total + down_in[l, o].astype(f32)
        result = (0.3 * values[...].astype(f32) + 0.5 * total * vectors[(0, 2)[l]]).astype(bf16)
        if l == 0:
            values[...] = result
        else:
            out[...] = result

    with scope("drain"):
        for l in range(2):
            for o in range(1, m):
                part_copy(l, o, x).wait_send()
            kept = core == cores - 1 if l == 0 else True

            @pl.when(jnp.logical_not(middle) & (kept | (p > 0)))
            def _():
                wait(sum_out.at[l], sum_ss.at[l])

            @pl.when(jnp.logical_not(middle))
            def _():
                wait(squares.at[l, pl.ds(0, 2)], sq_ss.at[l])

            for d in range(2):
                @pl.when(z == owners[d])
                def _():
                    wait(squares.at[l, 0], sq_ss.at[l])
                    wait(sum_out.at[l, pl.ds(0, counts[1 - d] * pieces)], sum_ss.at[l])
                    for dest in range(n):
                        if dest != owners[d]:
                            wait(hid.at[l, pl.ds(0, counts[d])], hid_ss.at[l, dest])


def per_device(n, m, cores, *args):
    tokens = args[0]
    rows, width = tokens.shape
    units = args[2].shape[1]
    pieces = 2 if units % (2 * LANES) == 0 else 1
    lanes = pieces * LANES
    blocks = units // lanes
    parts = units // LANES
    bf16, f32 = jnp.bfloat16, jnp.float32
    flat = [a if a.ndim > 1 else a.reshape(1, width) if i in (1, 7, 8, 14) else a.reshape(parts, LANES) for i, a in enumerate(args)]
    dma = pltpu.SemaphoreType.DMA
    return pl.pallas_call(
        functools.partial(kernel, (n, m, cores, rows, width, units, pieces, n * width)),
        out_shape=pltpu.VMEM((rows, width), bf16),
        in_specs=[pl.BlockSpec(memory_space=pl.ANY)] * len(flat),
        out_specs=pl.BlockSpec(memory_space=pltpu.VMEM),
        scratch_shapes=[
            pltpu.VMEM((rows, width), bf16),
            pltpu.VMEM((rows, width), bf16),
            pltpu.VMEM((4, 1, width), f32),
            pltpu.VMEM((4, parts, LANES), f32),
            pltpu.VMEM((2, blocks, width, 2 * lanes), f32),
            pltpu.VMEM((2, blocks, lanes, width), f32),
            pltpu.VMEM((parts, rows, 2 * LANES), f32),
            pltpu.VMEM((2, parts, rows, 2 * LANES), bf16),
            pltpu.VMEM((2, parts, rows, 2 * LANES), bf16),
            pltpu.VMEM((2, parts, rows, 2 * LANES), bf16),
            pltpu.VMEM((2, blocks, rows, lanes), bf16),
            pltpu.VMEM((rows, width), f32),
            pltpu.VMEM((2, m, rows, width), bf16),
            pltpu.VMEM((2, n, 8, rows), f32),
            pltpu.VMEM((rows, LANES), f32),
            dma((4,)),
            dma((blocks,)),
            dma((blocks,)),
            dma((2,)),
            dma((parts,)),
            dma(((blocks - blocks // 2) * pieces,)),
            dma((2, n)),
            dma((blocks,)),
            dma((2, m - 1)),
            dma((2, m - 1)),
            dma((2,)),
            dma,
            pltpu.SemaphoreType.REGULAR,
        ],
        compiler_params=pltpu.CompilerParams(
            collective_id=0, has_side_effects=True, vmem_limit_bytes=60 * 1024 * 1024
        ),
    )(*flat)


def solution(mesh):
    in_specs = (
        P(("grp", "dp"), "ra"),
        P("ra"),
        P("ra", "cb"),
        P("ra", "cb"),
        P("cb", "ra"),
        P("cb"),
        P("cb"),
        P("ra"),
        P("ra"),
        P("ra", "cb"),
        P("ra", "cb"),
        P("cb", "ra"),
        P("cb"),
        P("cb"),
        P("ra"),
    )
    out_specs = P(("grp", "dp"), "ra")
    n, m, cores = mesh.shape["ra"], mesh.shape["cb"], mesh.shape["dp"]
    return jax.shard_map(
        functools.partial(per_device, n, m, cores), mesh=mesh, in_specs=in_specs, out_specs=out_specs, check_vma=False
    )
```

```python
import functools

import jax
import jax.numpy as jnp
from jax import lax
from jax.experimental import pallas as pl
from jax.experimental.pallas import tpu as pltpu
from jax.sharding import PartitionSpec as P

EPS = 1e-06
MESH = pl.DeviceIdType.MESH
LANES = 128
LAG = 5


def kernel(dims, *refs):
    n, m, cores, rows, width, units, pieces, total_width = dims
    (tokens, gain0, gate0, up0, down0, gs0, us0, ds0, gain1, gate1, up1, down1, gs1, us1, ds1) = refs[:15]
    out = refs[15]
    (values, scaled, vectors, scales, w_gu, w_down, own, sum_out, sum_in, cross_in, hid, acc, down_in, squares, inverse,
     small_sem, gu_sem, sum_ss, sum_rs, cross_rs, hid_ss, hid_rs, part_ss, part_rs, sq_ss, sq_rs,
     turn_sem) = refs[16:]
    gate, up, down = (gate0, gate1), (up0, up1), (down0, down1)
    bf16, f32 = jnp.bfloat16, jnp.float32
    scope = jax.named_scope

    z, x, core = lax.axis_index("ra"), lax.axis_index("cb"), lax.axis_index("dp")
    lanes = pieces * LANES
    blocks = units // lanes
    half = n // 2
    owners = (half - 1, half)
    counts = (blocks - blocks // 2, blocks // 2)
    starts = (0, counts[0])
    left = z < half
    step = jnp.where(left, 1, -1)
    p = jnp.where(left, z, n - 1 - z)
    middle = (z == half - 1) | (z == half)
    first = jnp.where(left, counts[0], 0)
    n_far = jnp.where(left, counts[1], counts[0])
    n_near = blocks - n_far
    near_start = jnp.where(left, 0, counts[0])

    def wait(ref, sem):
        pltpu.make_async_copy(ref, ref, sem).wait()

    def columns(c):
        return pl.ds(pl.multiple_of(c * lanes, lanes), lanes)

    def gate_copy(l, c):
        return pltpu.make_async_copy(gate[l].at[:, columns(c)], w_gu.at[l, c, :, pl.ds(0, lanes)], gu_sem.at[c if l == 0 else blocks])

    def up_copy(l, c):
        return pltpu.make_async_copy(up[l].at[:, columns(c)], w_gu.at[l, c, :, pl.ds(lanes, lanes)], gu_sem.at[c if l == 0 else blocks])

    def down_copy(l, c):
        return pltpu.make_async_copy(down[l].at[columns(c), :], w_down.at[l, c], gu_sem.at[c if l == 0 else blocks + 1])

    def sum_copy(l, b):
        return pltpu.make_async_remote_copy(
            src_ref=sum_out.at[l, b], dst_ref=sum_in.at[l, b], send_sem=sum_ss.at[l], recv_sem=sum_rs.at[b],
            device_id={"ra": z + step}, device_id_type=MESH)

    def cross_copy(l, b):
        return pltpu.make_async_remote_copy(
            src_ref=sum_out.at[l, b], dst_ref=cross_in.at[l, b], send_sem=sum_ss.at[l],
            recv_sem=cross_rs.at[b - first * pieces], device_id={"ra": z + step}, device_id_type=MESH)

    def hid_copy(l, c, i, dest):
        part = hid.at[l, c, :, pl.ds(i * LANES, LANES)]
        return pltpu.make_async_remote_copy(
            src_ref=part, dst_ref=part, send_sem=hid_ss.at[l, dest], recv_sem=hid_rs.at[c],
            device_id={"ra": dest}, device_id_type=MESH)

    def part_copy(l, o, sender):
        return pltpu.make_async_remote_copy(
            src_ref=down_in.at[l, sender], dst_ref=down_in.at[l, sender], send_sem=part_ss.at[l, o - 1],
            recv_sem=part_rs.at[l, o - 1], device_id={"cb": lax.rem(x + o, m)}, device_id_type=MESH)

    def sq_copy(l, end, sender):
        return pltpu.make_async_remote_copy(
            src_ref=squares.at[l, sender], dst_ref=squares.at[l, sender], send_sem=sq_ss.at[l],
            recv_sem=sq_rs, device_id={"ra": owners[end]}, device_id_type=MESH)

    def others():
        return [jnp.where(left, n - 1 - o, o) + jnp.where(
            left, jnp.where(n - 1 - o <= z, -1, 0), jnp.where(o >= z, 1, 0)) for o in range(n - 1)]

    def stream(j):
        return lax.rem(first + j, blocks)

    def loop(low, high, step_fn):
        def one(i, carry):
            step_fn(i)
            return carry
        lax.fori_loop(low, high, one, 0)

    urgent = [pltpu.make_async_copy(tokens, values, small_sem.at[0]),
              pltpu.make_async_copy(gain0, vectors.at[3], small_sem.at[1])]
    for copy in urgent:
        copy.start()

    def start_first(i):
        c = stream(i)
        gate_copy(0, c).start()
        up_copy(0, c).start()

    loop(0, blocks, start_first)
    for i, src in enumerate((ds0, gain1, ds1)):
        pltpu.make_async_copy(src, vectors.at[i], small_sem.at[2]).start()
    for i, src in enumerate((gs0, gs1, us0, us1)):
        pltpu.make_async_copy(src, scales.at[i], small_sem.at[3]).start()

    barrier = pltpu.get_barrier_semaphore()

    def greet(device):
        pl.semaphore_signal(barrier, inc=1, device_id={"ra": device}, device_id_type=MESH)

    @pl.when(middle)
    def _():
        for o in range(1, n):
            greet(lax.rem(z + o, n))

    @pl.when(jnp.logical_not(middle))
    def _():
        for owner in owners:
            greet(owner)

        @pl.when(p < half - 2)
        def _():
            greet(z + step)

        @pl.when(p > 0)
        def _():
            greet(z - step)

    for o in range(1, m):
        pl.semaphore_signal(barrier, inc=1, device_id={"cb": lax.rem(x + o, m)}, device_id_type=MESH)
    for o in range(1, cores):
        pl.semaphore_signal(barrier, inc=1, device_id={"dp": lax.rem(core + o, cores)}, device_id_type=MESH)
    with scope("small"):
        for copy in urgent:
            copy.wait()

    for l in range(2):
        scaled[...] = (values[...].astype(f32) * vectors[(3, 1)[l]]).astype(bf16)
        if l == 0:
            with scope("barrier"):
                greeted = jnp.where(middle, n - 1, 2 + jnp.where(p < half - 2, 1, 0) + jnp.where(p > 0, 1, 0))
                pl.semaphore_wait(barrier, greeted + m + cores - 2)

        def product(k, store):
            c = stream(k)
            if l == 0:
                with scope("w_gu"):
                    wait(w_gu.at[l, c], gu_sem.at[c])
                down_copy(0, c).start()
            both = jnp.dot(scaled[...], w_gu[l, c].astype(bf16), preferred_element_type=f32)
            for i in range(pieces):
                a, b = i * LANES, lanes + i * LANES
                store(c * pieces + i, both[:, a:a + LANES], both[:, b:b + LANES])

        if l == 1:
            wait(w_gu.at[1], gu_sem.at[blocks])

        def send_squares(k):
            @pl.when(k == 2)
            def _():
                floats = values[...].astype(f32)
                squares[l, z] = lax.dot_general(
                    jnp.ones((8, width), f32), floats * floats, (((1,), (1,)), ((), ())),
                    precision=lax.Precision.HIGHEST, preferred_element_type=f32)
                for end in range(2):
                    @pl.when(z != owners[end])
                    def _():
                        sq_copy(l, end, z).start()

        def fetch_second():
            if l == 0:
                def one(k):
                    c = stream(k)
                    gate_copy(1, c).start()
                    up_copy(1, c).start()
                loop(0, blocks, one)

        def use_hidden(c):
            if l == 0:
                down_copy(l, c).wait()
            acc[...] += jnp.dot(hid[l, c], w_down[l, c].astype(bf16), preferred_element_type=f32)

        def wait_hidden(c):
            with scope("w_hid"):
                wait(hid.at[l, c], hid_rs.at[c])

        def to_out(b, g, u):
            sum_out[l, b, :, :LANES] = g.astype(bf16)
            sum_out[l, b, :, LANES:] = u.astype(bf16)

        def to_own(b, g, u):
            own[b, :, :LANES] = g
            own[b, :, LANES:] = u

        def pass_on(b, copy):
            with scope("w_sum"):
                sum_copy(l, b).wait_recv()
            sum_out[l, b] = (own[b] + sum_in[l, b].astype(f32)).astype(bf16)
            copy(l, b).start()

        @pl.when(jnp.logical_not(middle))
        def _():
            @pl.when(p == 0)
            def _():
                def make(k):
                    product(k, to_out)
                    send = [sum_copy(l, stream(k) * pieces + i) for i in range(pieces)]
                    if l == 0:
                        @pl.when(core == 0)
                        def _():
                            for copy in send:
                                copy.start()
                    else:
                        for copy in send:
                            copy.start()
                    send_squares(k)

                with scope("make"):
                    loop(0, blocks, make)
                fetch_second()
                if l == 0:
                    @pl.when(core > 0)
                    def _():
                        with scope("turn"):
                            pl.semaphore_wait(turn_sem, 1)

                        def one(k):
                            for i in range(pieces):
                                sum_copy(l, stream(k) * pieces + i).start()
                        loop(0, blocks, one)

                    @pl.when(core < cores - 1)
                    def _():
                        with scope("held"):
                            wait(sum_out.at[l], sum_ss.at[l])
                        pl.semaphore_signal(turn_sem, inc=1, device_id={"dp": core + 1}, device_id_type=MESH)

            @pl.when(p > 0)
            def _():
                def relay(k):
                    product(k, to_own)
                    send_squares(k)
                    for i in range(pieces):
                        pass_on(stream(k) * pieces + i, sum_copy)

                loop(0, blocks, relay)
                fetch_second()

            acc[...] = jnp.zeros_like(acc)
            if l == 1:
                wait(w_down.at[1], gu_sem.at[blocks + 1])

            lead = jnp.where(left, counts[0] - counts[1], 0)

            def take(c):
                wait_hidden(c)
                use_hidden(c)

            def gather(k):
                @pl.when(k + lead < counts[0])
                def _():
                    take(starts[0] + k + lead)

                @pl.when(k < counts[1])
                def _():
                    take(starts[1] + k)

            with scope("gather"):
                loop(0, lead, lambda k: take(starts[0] + k))
                loop(0, counts[0], gather)

        @pl.when(middle)
        def _():
            ahead = blocks // 2

            def make(k):
                product(k, to_own)
                send_squares(k)

            with scope("make"):
                loop(0, ahead, make)

            def far(k):
                make(k)

                @pl.when(k - ahead < n_far)
                def _():
                    for i in range(pieces):
                        b = stream(k - ahead) * pieces + i
                        if half == 1:
                            sum_out[l, b] = own[b].astype(bf16)
                            cross_copy(l, b).start()
                        else:
                            pass_on(b, cross_copy)

            with scope("far"):
                loop(ahead, blocks, far)
            fetch_second()
            acc[...] = jnp.zeros_like(acc)
            if l == 1:
                wait(w_down.at[1], gu_sem.at[blocks + 1])
            with scope("w_sq"):
                wait(squares.at[l, pl.ds(0, n - 1)], sq_rs)
            every = squares[l].reshape(8 * n, rows)
            total = lax.dot_general(
                every, jnp.full((8 * n, LANES), 0.125, f32), (((0,), (0,)), ((), ())),
                precision=lax.Precision.HIGHEST, preferred_element_type=f32)
            inverse[...] = lax.rsqrt(total / total_width + EPS)
            if l == 0:
                with scope("w_small"):
                    wait(scales, small_sem.at[3])

            def near(s):
                @pl.when(s < n_near)
                def _():
                    c = near_start + s
                    for i in range(pieces):
                        b = c * pieces + i
                        both = own[b]
                        if half > 1:
                            with scope("w_sum"):
                                sum_copy(l, b).wait_recv()
                            both = both + sum_in[l, b].astype(f32)
                        with scope("w_cross"):
                            wait(cross_in.at[l, b], cross_rs.at[b - near_start * pieces])
                        both = both + cross_in[l, b].astype(f32)
                        inv = inverse[...]
                        g = both[:, :LANES] * scales[l, pl.ds(b, 1), :] * inv
                        u = both[:, LANES:] * scales[2 + l, pl.ds(b, 1), :] * inv
                        hid[l, c, :, i * LANES:(i + 1) * LANES] = (g / (1.0 + jnp.exp(-g)) * u).astype(bf16)
                        for dest in others():
                            hid_copy(l, c, i, dest).start()
                    use_hidden(c)

                k = s - LAG

                @pl.when((k >= 0) & (k < n_far))
                def _():
                    wait_hidden(first + k)
                    use_hidden(first + k)

            with scope("near"):
                loop(0, counts[0] + LAG, near)

        down_in[l, x] = acc[...].astype(bf16)
        for o in range(1, m):
            part_copy(l, o, x).start()
        if l == 0:
            loop(0, blocks, lambda k: down_copy(1, k).start())
            wait(vectors.at[pl.ds(0, 3)], small_sem.at[2])

            @pl.when(jnp.logical_not(middle))
            def _():
                wait(scales, small_sem.at[3])
        with scope("exch"):
            for o in range(1, m):
                part_copy(l, o, lax.rem(x - o + m, m)).wait_recv()
        total = down_in[l, 0].astype(f32)
        for o in range(1, m):
            total = total + down_in[l, o].astype(f32)
        result = (0.3 * values[...].astype(f32) + 0.5 * total * vectors[(0, 2)[l]]).astype(bf16)
        if l == 0:
            values[...] = result
        else:
            out[...] = result

    with scope("drain"):
        for l in range(2):
            for o in range(1, m):
                part_copy(l, o, x).wait_send()
            kept = core == cores - 1 if l == 0 else True

            @pl.when(jnp.logical_not(middle) & (kept | (p > 0)))
            def _():
                wait(sum_out.at[l], sum_ss.at[l])

            @pl.when(jnp.logical_not(middle))
            def _():
                wait(squares.at[l, pl.ds(0, 2)], sq_ss.at[l])

            for d in range(2):
                @pl.when(z == owners[d])
                def _():
                    wait(squares.at[l, 0], sq_ss.at[l])
                    wait(sum_out.at[l, pl.ds(0, counts[1 - d] * pieces)], sum_ss.at[l])
                    for dest in range(n):
                        if dest != owners[d]:
                            wait(hid.at[l, pl.ds(0, counts[d])], hid_ss.at[l, dest])


def per_device(n, m, cores, *args):
    tokens = args[0]
    rows, width = tokens.shape
    units = args[2].shape[1]
    pieces = 2 if units % (2 * LANES) == 0 else 1
    lanes = pieces * LANES
    blocks = units // lanes
    parts = units // LANES
    bf16, f32 = jnp.bfloat16, jnp.float32
    flat = [a if a.ndim > 1 else a.reshape(1, width) if i in (1, 7, 8, 14) else a.reshape(parts, LANES) for i, a in enumerate(args)]
    dma = pltpu.SemaphoreType.DMA
    return pl.pallas_call(
        functools.partial(kernel, (n, m, cores, rows, width, units, pieces, n * width)),
        out_shape=pltpu.VMEM((rows, width), bf16),
        in_specs=[pl.BlockSpec(memory_space=pl.ANY)] * len(flat),
        out_specs=pl.BlockSpec(memory_space=pltpu.VMEM),
        scratch_shapes=[
            pltpu.VMEM((rows, width), bf16),
            pltpu.VMEM((rows, width), bf16),
            pltpu.VMEM((4, 1, width), f32),
            pltpu.VMEM((4, parts, LANES), f32),
            pltpu.VMEM((2, blocks, width, 2 * lanes), f32),
            pltpu.VMEM((2, blocks, lanes, width), f32),
            pltpu.VMEM((parts, rows, 2 * LANES), f32),
            pltpu.VMEM((2, parts, rows, 2 * LANES), bf16),
            pltpu.VMEM((2, parts, rows, 2 * LANES), bf16),
            pltpu.VMEM((2, parts, rows, 2 * LANES), bf16),
            pltpu.VMEM((2, blocks, rows, lanes), bf16),
            pltpu.VMEM((rows, width), f32),
            pltpu.VMEM((2, m, rows, width), bf16),
            pltpu.VMEM((2, n, 8, rows), f32),
            pltpu.VMEM((rows, LANES), f32),
            dma((4,)),
            dma((blocks + 2,)),
            dma((2,)),
            dma((parts,)),
            dma(((blocks - blocks // 2) * pieces,)),
            dma((2, n)),
            dma((blocks,)),
            dma((2, m - 1)),
            dma((2, m - 1)),
            dma((2,)),
            dma,
            pltpu.SemaphoreType.REGULAR,
        ],
        compiler_params=pltpu.CompilerParams(
            collective_id=0, has_side_effects=True, vmem_limit_bytes=60 * 1024 * 1024
        ),
    )(*flat)


def solution(mesh):
    in_specs = (
        P(("grp", "dp"), "ra"),
        P("ra"),
        P("ra", "cb"),
        P("ra", "cb"),
        P("cb", "ra"),
        P("cb"),
        P("cb"),
        P("ra"),
        P("ra"),
        P("ra", "cb"),
        P("ra", "cb"),
        P("cb", "ra"),
        P("cb"),
        P("cb"),
        P("ra"),
    )
    out_specs = P(("grp", "dp"), "ra")
    n, m, cores = mesh.shape["ra"], mesh.shape["cb"], mesh.shape["dp"]
    return jax.shard_map(
        functools.partial(per_device, n, m, cores), mesh=mesh, in_specs=in_specs, out_specs=out_specs, check_vma=False
    )
```

```python
import functools

import jax
import jax.numpy as jnp
from jax import lax
from jax.experimental import pallas as pl
from jax.experimental.pallas import tpu as pltpu
from jax.sharding import PartitionSpec as P

EPS = 1e-06
MESH = pl.DeviceIdType.MESH
LANES = 128
LAG = 5


def kernel(dims, *refs):
    n, m, cores, rows, width, units, pieces, total_width = dims
    (tokens, gain0, gate0, up0, down0, gs0, us0, ds0, gain1, gate1, up1, down1, gs1, us1, ds1) = refs[:15]
    out = refs[15]
    (values, scaled, vectors, scales, w_gu, w_down, own, sum_out, sum_in, cross_in, hid, acc, down_in, squares, inverse,
     small_sem, gu_sem, sum_ss, sum_rs, cross_rs, hid_ss, hid_rs, part_ss, part_rs, sq_ss, sq_rs,
     turn_sem) = refs[16:]
    gate, up, down = (gate0, gate1), (up0, up1), (down0, down1)
    bf16, f32 = jnp.bfloat16, jnp.float32
    scope = jax.named_scope

    z, x, core = lax.axis_index("ra"), lax.axis_index("cb"), lax.axis_index("dp")
    lanes = pieces * LANES
    blocks = units // lanes
    half = n // 2
    owners = (half - 1, half)
    counts = (blocks - blocks // 2, blocks // 2)
    starts = (0, counts[0])
    left = z < half
    step = jnp.where(left, 1, -1)
    p = jnp.where(left, z, n - 1 - z)
    middle = (z == half - 1) | (z == half)
    first = jnp.where(left, counts[0], 0)
    n_far = jnp.where(left, counts[1], counts[0])
    n_near = blocks - n_far
    near_start = jnp.where(left, 0, counts[0])

    def wait(ref, sem):
        pltpu.make_async_copy(ref, ref, sem).wait()

    def columns(c):
        return pl.ds(pl.multiple_of(c * lanes, lanes), lanes)

    def gate_copy(l, c):
        return pltpu.make_async_copy(gate[l].at[:, columns(c)], w_gu.at[l, c, :, pl.ds(0, lanes)], gu_sem.at[c if l == 0 else blocks])

    def up_copy(l, c):
        return pltpu.make_async_copy(up[l].at[:, columns(c)], w_gu.at[l, c, :, pl.ds(lanes, lanes)], gu_sem.at[c if l == 0 else blocks])

    def down_copy(l, c):
        return pltpu.make_async_copy(down[l].at[columns(c), :], w_down.at[l, c], gu_sem.at[c if l == 0 else blocks + 1])

    def sum_copy(l, b):
        return pltpu.make_async_remote_copy(
            src_ref=sum_out.at[l, b], dst_ref=sum_in.at[l, b], send_sem=sum_ss.at[l], recv_sem=sum_rs.at[b],
            device_id={"ra": z + step}, device_id_type=MESH)

    def cross_copy(l, b):
        return pltpu.make_async_remote_copy(
            src_ref=sum_out.at[l, b], dst_ref=cross_in.at[l, b], send_sem=sum_ss.at[l],
            recv_sem=cross_rs.at[b - first * pieces], device_id={"ra": z + step}, device_id_type=MESH)

    def hid_copy(l, c, i, dest):
        part = hid.at[l, c, :, pl.ds(i * LANES, LANES)]
        return pltpu.make_async_remote_copy(
            src_ref=part, dst_ref=part, send_sem=hid_ss.at[l, dest], recv_sem=hid_rs.at[c],
            device_id={"ra": dest}, device_id_type=MESH)

    def part_copy(l, o, sender):
        return pltpu.make_async_remote_copy(
            src_ref=down_in.at[l, sender], dst_ref=down_in.at[l, sender], send_sem=part_ss.at[l, o - 1],
            recv_sem=part_rs.at[l, o - 1], device_id={"cb": lax.rem(x + o, m)}, device_id_type=MESH)

    def sq_copy(l, end, sender):
        return pltpu.make_async_remote_copy(
            src_ref=squares.at[l, sender], dst_ref=squares.at[l, sender], send_sem=sq_ss.at[l],
            recv_sem=sq_rs, device_id={"ra": owners[end]}, device_id_type=MESH)

    def others():
        return [jnp.where(left, n - 1 - o, o) + jnp.where(
            left, jnp.where(n - 1 - o <= z, -1, 0), jnp.where(o >= z, 1, 0)) for o in range(n - 1)]

    def stream(j):
        return lax.rem(first + j, blocks)

    def loop(low, high, step_fn):
        def one(i, carry):
            step_fn(i)
            return carry
        lax.fori_loop(low, high, one, 0)

    barrier = pltpu.get_barrier_semaphore()

    def greet(device):
        pl.semaphore_signal(barrier, inc=1, device_id={"ra": device}, device_id_type=MESH)

    @pl.when(middle)
    def _():
        for o in range(1, n):
            greet(lax.rem(z + o, n))

    @pl.when(jnp.logical_not(middle))
    def _():
        for owner in owners:
            greet(owner)

        @pl.when(p < half - 2)
        def _():
            greet(z + step)

        @pl.when(p > 0)
        def _():
            greet(z - step)

    for o in range(1, m):
        pl.semaphore_signal(barrier, inc=1, device_id={"cb": lax.rem(x + o, m)}, device_id_type=MESH)
    for o in range(1, cores):
        pl.semaphore_signal(barrier, inc=1, device_id={"dp": lax.rem(core + o, cores)}, device_id_type=MESH)
    urgent = [pltpu.make_async_copy(tokens, values, small_sem.at[0]),
              pltpu.make_async_copy(gain0, vectors.at[3], small_sem.at[1])]
    for copy in urgent:
        copy.start()

    def start_first(i):
        c = stream(i)
        gate_copy(0, c).start()
        up_copy(0, c).start()

    loop(0, blocks, start_first)
    for i, src in enumerate((ds0, gain1, ds1)):
        pltpu.make_async_copy(src, vectors.at[i], small_sem.at[2]).start()
    for i, src in enumerate((gs0, gs1, us0, us1)):
        pltpu.make_async_copy(src, scales.at[i], small_sem.at[3]).start()

    with scope("small"):
        for copy in urgent:
            copy.wait()

    for l in range(2):
        scaled[...] = (values[...].astype(f32) * vectors[(3, 1)[l]]).astype(bf16)
        if l == 0:
            with scope("barrier"):
                greeted = jnp.where(middle, n - 1, 2 + jnp.where(p < half - 2, 1, 0) + jnp.where(p > 0, 1, 0))
                pl.semaphore_wait(barrier, greeted + m + cores - 2)

        def product(k, store):
            c = stream(k)
            if l == 0:
                with scope("w_gu"):
                    wait(w_gu.at[l, c], gu_sem.at[c])
                down_copy(0, c).start()
            both = jnp.dot(scaled[...], w_gu[l, c].astype(bf16), preferred_element_type=f32)
            for i in range(pieces):
                a, b = i * LANES, lanes + i * LANES
                store(c * pieces + i, both[:, a:a + LANES], both[:, b:b + LANES])

        if l == 1:
            wait(w_gu.at[1], gu_sem.at[blocks])

        def send_squares(k):
            @pl.when(k == 2)
            def _():
                floats = values[...].astype(f32)
                squares[l, z] = lax.dot_general(
                    jnp.ones((8, width), f32), floats * floats, (((1,), (1,)), ((), ())),
                    precision=lax.Precision.HIGHEST, preferred_element_type=f32)
                for end in range(2):
                    @pl.when(z != owners[end])
                    def _():
                        sq_copy(l, end, z).start()

        def fetch_second():
            if l == 0:
                def one(k):
                    c = stream(k)
                    gate_copy(1, c).start()
                    up_copy(1, c).start()
                loop(0, blocks, one)

        def use_hidden(c):
            if l == 0:
                down_copy(l, c).wait()
            acc[...] += jnp.dot(hid[l, c], w_down[l, c].astype(bf16), preferred_element_type=f32)

        def wait_hidden(c):
            with scope("w_hid"):
                wait(hid.at[l, c], hid_rs.at[c])

        def to_out(b, g, u):
            sum_out[l, b, :, :LANES] = g.astype(bf16)
            sum_out[l, b, :, LANES:] = u.astype(bf16)

        def to_own(b, g, u):
            own[b, :, :LANES] = g
            own[b, :, LANES:] = u

        def pass_on(b, copy):
            with scope("w_sum"):
                sum_copy(l, b).wait_recv()
            sum_out[l, b] = (own[b] + sum_in[l, b].astype(f32)).astype(bf16)
            copy(l, b).start()

        @pl.when(jnp.logical_not(middle))
        def _():
            @pl.when(p == 0)
            def _():
                def make(k):
                    product(k, to_out)
                    send = [sum_copy(l, stream(k) * pieces + i) for i in range(pieces)]
                    if l == 0:
                        @pl.when(core == 0)
                        def _():
                            for copy in send:
                                copy.start()
                    else:
                        for copy in send:
                            copy.start()
                    send_squares(k)

                with scope("make"):
                    loop(0, blocks, make)
                fetch_second()
                if l == 0:
                    @pl.when(core > 0)
                    def _():
                        with scope("turn"):
                            pl.semaphore_wait(turn_sem, 1)

                        def one(k):
                            for i in range(pieces):
                                sum_copy(l, stream(k) * pieces + i).start()
                        loop(0, blocks, one)

                    @pl.when(core < cores - 1)
                    def _():
                        with scope("held"):
                            wait(sum_out.at[l], sum_ss.at[l])
                        pl.semaphore_signal(turn_sem, inc=1, device_id={"dp": core + 1}, device_id_type=MESH)

            @pl.when(p > 0)
            def _():
                def relay(k):
                    product(k, to_own)
                    send_squares(k)
                    for i in range(pieces):
                        pass_on(stream(k) * pieces + i, sum_copy)

                loop(0, blocks, relay)
                fetch_second()

            acc[...] = jnp.zeros_like(acc)
            if l == 1:
                wait(w_down.at[1], gu_sem.at[blocks + 1])

            lead = jnp.where(left, counts[0] - counts[1], 0)

            def take(c):
                wait_hidden(c)
                use_hidden(c)

            def gather(k):
                @pl.when(k + lead < counts[0])
                def _():
                    take(starts[0] + k + lead)

                @pl.when(k < counts[1])
                def _():
                    take(starts[1] + k)

            with scope("gather"):
                loop(0, lead, lambda k: take(starts[0] + k))
                loop(0, counts[0], gather)

        @pl.when(middle)
        def _():
            ahead = blocks // 2

            def make(k):
                product(k, to_own)
                send_squares(k)

            with scope("make"):
                loop(0, ahead, make)

            def far(k):
                make(k)

                @pl.when(k - ahead < n_far)
                def _():
                    for i in range(pieces):
                        b = stream(k - ahead) * pieces + i
                        if half == 1:
                            sum_out[l, b] = own[b].astype(bf16)
                            cross_copy(l, b).start()
                        else:
                            pass_on(b, cross_copy)

            with scope("far"):
                loop(ahead, blocks, far)
            fetch_second()
            acc[...] = jnp.zeros_like(acc)
            if l == 1:
                wait(w_down.at[1], gu_sem.at[blocks + 1])
            with scope("w_sq"):
                wait(squares.at[l, pl.ds(0, n - 1)], sq_rs)
            every = squares[l].reshape(8 * n, rows)
            total = lax.dot_general(
                every, jnp.full((8 * n, LANES), 0.125, f32), (((0,), (0,)), ((), ())),
                precision=lax.Precision.HIGHEST, preferred_element_type=f32)
            inverse[...] = lax.rsqrt(total / total_width + EPS)
            if l == 0:
                with scope("w_small"):
                    wait(scales, small_sem.at[3])

            def near(s):
                @pl.when(s < n_near)
                def _():
                    c = near_start + s
                    for i in range(pieces):
                        b = c * pieces + i
                        both = own[b]
                        if half > 1:
                            with scope("w_sum"):
                                sum_copy(l, b).wait_recv()
                            both = both + sum_in[l, b].astype(f32)
                        with scope("w_cross"):
                            wait(cross_in.at[l, b], cross_rs.at[b - near_start * pieces])
                        both = both + cross_in[l, b].astype(f32)
                        inv = inverse[...]
                        g = both[:, :LANES] * scales[l, pl.ds(b, 1), :] * inv
                        u = both[:, LANES:] * scales[2 + l, pl.ds(b, 1), :] * inv
                        hid[l, c, :, i * LANES:(i + 1) * LANES] = (g / (1.0 + jnp.exp(-g)) * u).astype(bf16)
                        for dest in others():
                            hid_copy(l, c, i, dest).start()
                    use_hidden(c)

                k = s - LAG

                @pl.when((k >= 0) & (k < n_far))
                def _():
                    wait_hidden(first + k)
                    use_hidden(first + k)

            with scope("near"):
                loop(0, counts[0] + LAG, near)

        down_in[l, x] = acc[...].astype(bf16)
        for o in range(1, m):
            part_copy(l, o, x).start()
        if l == 0:
            loop(0, blocks, lambda k: down_copy(1, k).start())
            wait(vectors.at[pl.ds(0, 3)], small_sem.at[2])

            @pl.when(jnp.logical_not(middle))
            def _():
                wait(scales, small_sem.at[3])
        with scope("exch"):
            for o in range(1, m):
                part_copy(l, o, lax.rem(x - o + m, m)).wait_recv()
        total = down_in[l, 0].astype(f32)
        for o in range(1, m):
            total = total + down_in[l, o].astype(f32)
        result = (0.3 * values[...].astype(f32) + 0.5 * total * vectors[(0, 2)[l]]).astype(bf16)
        if l == 0:
            values[...] = result
        else:
            out[...] = result

    with scope("drain"):
        for l in range(2):
            for o in range(1, m):
                part_copy(l, o, x).wait_send()
            kept = core == cores - 1 if l == 0 else True

            @pl.when(jnp.logical_not(middle) & (kept | (p > 0)))
            def _():
                wait(sum_out.at[l], sum_ss.at[l])

            @pl.when(jnp.logical_not(middle))
            def _():
                wait(squares.at[l, pl.ds(0, 2)], sq_ss.at[l])

            for d in range(2):
                @pl.when(z == owners[d])
                def _():
                    wait(squares.at[l, 0], sq_ss.at[l])
                    wait(sum_out.at[l, pl.ds(0, counts[1 - d] * pieces)], sum_ss.at[l])
                    for dest in range(n):
                        if dest != owners[d]:
                            wait(hid.at[l, pl.ds(0, counts[d])], hid_ss.at[l, dest])


def per_device(n, m, cores, *args):
    tokens = args[0]
    rows, width = tokens.shape
    units = args[2].shape[1]
    pieces = 2 if units % (2 * LANES) == 0 else 1
    lanes = pieces * LANES
    blocks = units // lanes
    parts = units // LANES
    bf16, f32 = jnp.bfloat16, jnp.float32
    flat = [a if a.ndim > 1 else a.reshape(1, width) if i in (1, 7, 8, 14) else a.reshape(parts, LANES) for i, a in enumerate(args)]
    dma = pltpu.SemaphoreType.DMA
    return pl.pallas_call(
        functools.partial(kernel, (n, m, cores, rows, width, units, pieces, n * width)),
        out_shape=pltpu.VMEM((rows, width), bf16),
        in_specs=[pl.BlockSpec(memory_space=pl.ANY)] * len(flat),
        out_specs=pl.BlockSpec(memory_space=pltpu.VMEM),
        scratch_shapes=[
            pltpu.VMEM((rows, width), bf16),
            pltpu.VMEM((rows, width), bf16),
            pltpu.VMEM((4, 1, width), f32),
            pltpu.VMEM((4, parts, LANES), f32),
            pltpu.VMEM((2, blocks, width, 2 * lanes), f32),
            pltpu.VMEM((2, blocks, lanes, width), f32),
            pltpu.VMEM((parts, rows, 2 * LANES), f32),
            pltpu.VMEM((2, parts, rows, 2 * LANES), bf16),
            pltpu.VMEM((2, parts, rows, 2 * LANES), bf16),
            pltpu.VMEM((2, parts, rows, 2 * LANES), bf16),
            pltpu.VMEM((2, blocks, rows, lanes), bf16),
            pltpu.VMEM((rows, width), f32),
            pltpu.VMEM((2, m, rows, width), bf16),
            pltpu.VMEM((2, n, 8, rows), f32),
            pltpu.VMEM((rows, LANES), f32),
            dma((4,)),
            dma((blocks + 2,)),
            dma((2,)),
            dma((parts,)),
            dma(((blocks - blocks // 2) * pieces,)),
            dma((2, n)),
            dma((blocks,)),
            dma((2, m - 1)),
            dma((2, m - 1)),
            dma((2,)),
            dma,
            pltpu.SemaphoreType.REGULAR,
        ],
        compiler_params=pltpu.CompilerParams(
            collective_id=0, has_side_effects=True, vmem_limit_bytes=60 * 1024 * 1024
        ),
    )(*flat)


def solution(mesh):
    in_specs = (
        P(("grp", "dp"), "ra"),
        P("ra"),
        P("ra", "cb"),
        P("ra", "cb"),
        P("cb", "ra"),
        P("cb"),
        P("cb"),
        P("ra"),
        P("ra"),
        P("ra", "cb"),
        P("ra", "cb"),
        P("cb", "ra"),
        P("cb"),
        P("cb"),
        P("ra"),
    )
    out_specs = P(("grp", "dp"), "ra")
    n, m, cores = mesh.shape["ra"], mesh.shape["cb"], mesh.shape["dp"]
    return jax.shard_map(
        functools.partial(per_device, n, m, cores), mesh=mesh, in_specs=in_specs, out_specs=out_specs, check_vma=False
    )
```
